32 devices in a mesh: ep: 8 (over z, x), tp: 4 (over y, core).
Axes of the slice: x: 2, y: 2, z: 4, core: 2. Of those that a mesh axis runs over, the one named last changes fastest.
Arguments:
- tokens: bfloat16 [1536, 2048], P('ep'), may hold values from -6 to 6
- cotangent: bfloat16 [1536, 2048], P('ep'), may hold values from -6 to 6
- routing: int32 [1536, 2], P('ep'), may hold values from 0 to 7, all different within a row; in each aligned block of 192 rows (0 to 191, 192 to 383, ...) at most 60 rows name the same one
- route_weights: float32 [1536, 2], P('ep'), may hold values from 0.1 to 1
- w_gate: bfloat16 [8, 2048, 2048], P('ep', None, 'tp'), may hold values from -0.125 to 0.125
- w_up: bfloat16 [8, 2048, 2048], P('ep', None, 'tp'), may hold values from -0.125 to 0.125
- w_down: bfloat16 [8, 2048, 2048], P('ep', 'tp'), may hold values from -0.125 to 0.125
Outputs:
- grad_tokens: bfloat16 [1536, 2048], P('ep')
- grad_weights: bfloat16 [1536, 2], P('ep')
- grad_gate: bfloat16 [8, 2048, 2048], P('ep', None, 'tp')
- grad_up: bfloat16 [8, 2048, 2048], P('ep', None, 'tp')
- grad_down: bfloat16 [8, 2048, 2048], P('ep', 'tp')
The draws below stay inside these ranges and needn't reach their ends.
Inputs may be any that keep to these rules, and one draw needn't show every extreme that they name: `routing`: each row names 2 different experts. Within the rows of one device no expert is named more than 60 times, and in every draw some expert is named exactly 60 times by some device's rows.
All inputs are finite; a program needn't handle non-finite values.
Results may differ from the reference program's by a relative error of at most 0.019.
Values may be sent and summed in bfloat16 or wider, within the bound.
A program may use at most 64 MiB of HBM per device.

```python
import math
import jax
import jax.numpy as jnp
import numpy as np
from jax import lax

D = 2048
F = 2048
TOP = 2
TOK_DEV = 192
EXPERTS = 8
CAP = 60
TOKENS = 1536
N_EP = 8
N_TP = 4


def levels(stream_key, dims, cuts, least, top_value):
    gain, own = 1.0, jax.random.fold_in(stream_key, 6)
    for axis_at, blocks in cuts:
        draws = jnp.exp(jax.random.uniform(jax.random.fold_in(own, axis_at), (blocks,), jnp.float32, least / len(cuts), top_value / len(cuts)))
        gain = gain * jnp.repeat(draws, dims[axis_at] // blocks).reshape([-1 if axis == axis_at else 1 for axis in range(len(dims))])
    return gain


def deal_out(key, own, number, rows, amount, top, most, lean):
    ranking = jax.random.permutation(key, amount)
    packed, ordinary = portions_of(amount, rows * top, most, lean, True), portions_of(amount, rows * top, most, lean, False)
    places = jnp.arange(amount)

    def named(lengths, turn):
        used = int((lengths > 0).sum())
        fixed = max(1, used // 4)
        shifted = fixed + (places - fixed + turn * (used - fixed)) % max(1, amount - fixed)
        return jnp.zeros((amount,), jnp.int32).at[ranking[jnp.where(places < fixed, places, shifted)]].set(jnp.asarray(lengths, jnp.int32))

    lengths = jnp.where(number % 4 == 0, named(packed, number // 4), named(ordinary, number - number // 4 - 1))
    mixed = jax.random.permutation(jax.random.fold_in(own, 3), amount)
    donor, sink = mixed[0:amount // 2 * 2:2], mixed[1:amount // 2 * 2:2]
    room = jnp.minimum(lengths[donor] - 1, most - lengths[sink]) // 2
    room = jnp.where((donor == ranking[0]) | (sink == ranking[0]) | (lengths[sink] == 0), 0, jnp.maximum(room, 0))
    shifted = jax.random.randint(jax.random.fold_in(own, 4), (amount // 2,), 0, 1 << 20) % (room + 1)
    lengths = lengths.at[donor].add(-shifted).at[sink].add(shifted)
    members = jnp.searchsorted(jnp.cumsum(lengths), jnp.arange(rows * top), side="right").astype(jnp.int32)
    grid = members.reshape(top, rows).T
    grid = grid[jax.random.permutation(jax.random.fold_in(own, 1), rows)]
    turn = jax.random.randint(jax.random.fold_in(own, 2), (rows, 1), 0, top)
    return jnp.take_along_axis(grid, (jnp.arange(top)[None, :] + turn) % top, axis=1)


def portions_of(count, total, most, lean, full):
    loads = [(1 << 20) // math.isqrt(grade ** lean) + 1 for grade in range(1, count + 1)]
    largest = most if full else min(most, max(-(-total // count), total * loads[0] // sum(loads)))
    least = 1 if total - largest >= count - 1 else 0
    holding, surplus = [largest] + [least] * (count - 1), total - largest - least * (count - 1)
    while surplus > 0:
        candidates = [i for i in range(1, count) if holding[i] < largest] or [i for i in range(1, count) if holding[i] < most]
        pool, remaining = sum([loads[i] for i in candidates]), surplus
        for i in candidates:
            more = min(most - holding[i], max(1, remaining * loads[i] // pool), surplus)
            holding[i] = holding[i] + more
            surplus = surplus - more
    return np.array(holding)


def noise(key, extent, spread, most, cuts=(), kind=jnp.bfloat16):
    factor_of = levels(key, extent, cuts, -0.22, 0.18) if cuts else 1.0
    drawn = jax.random.normal(key, extent, jnp.float32) * spread * factor_of
    return jnp.minimum(jnp.maximum(drawn, -most), most).astype(kind)


def setup_inputs(seed: int = 0) -> dict:
    keys = jax.random.split(jax.random.key(seed), 8)
    tokens = noise(keys[0], (TOKENS, D), 1.0, 6.0, ((0, 8),))
    cotangent = noise(keys[1], (TOKENS, D), 1.0, 6.0, ((0, 8),))
    routing_keys = jax.random.split(jax.random.fold_in(keys[2], 1), TOKENS // TOK_DEV)
    routing_turns = jax.random.permutation(jax.random.fold_in(keys[2], 3), TOKENS // TOK_DEV)
    routing = jax.vmap(lambda own, number: deal_out(jax.random.fold_in(keys[2], 2), own, number, TOK_DEV, EXPERTS, TOP, CAP, 2))(routing_keys, routing_turns).reshape((TOKENS, TOP))
    route_weights = jnp.clip(jnp.exp(math.log(1.0) - 2.3025851 * jax.random.uniform(keys[3], (TOKENS, TOP), jnp.float32) ** levels(keys[3], (TOKENS, TOP), ((0, 8),), -0.2, 0.2)), 0.1, 1.0)
    w_gate = noise(keys[4], (EXPERTS, D, F), D ** -0.5, 0.125, ((0, 8), (2, 4)))
    w_up = noise(keys[5], (EXPERTS, D, F), D ** -0.5, 0.125, ((0, 8), (2, 4)))
    w_down = noise(keys[6], (EXPERTS, F, D), F ** -0.5, 0.125, ((0, 8), (1, 4)))
    return {"tokens": tokens, "cotangent": cotangent, "routing": routing, "route_weights": route_weights, "w_gate": w_gate, "w_up": w_up, "w_down": w_down}


def reference(tokens, cotangent, routing, route_weights, w_gate, w_up, w_down):
    all_tokens = tokens.shape[0]
    experts = EXPERTS
    blocks = routing.reshape(N_EP, TOK_DEV * TOP)
    onehot = (blocks[:, :, None] == jnp.arange(experts, dtype=jnp.int32)[None, None, :]).astype(jnp.int32)
    before = jnp.cumsum(onehot, axis=1) - onehot
    within = jnp.sum(before * onehot, axis=2)
    source = jnp.arange(N_EP, dtype=jnp.int32)[:, None]
    place = (source * CAP + within).reshape(-1).astype(jnp.int32)
    expert_of = routing.reshape(-1).astype(jnp.int32)
    token_of = jnp.repeat(jnp.arange(all_tokens, dtype=jnp.int32), TOP)
    slot_count = N_EP * CAP
    table = jnp.full((experts, slot_count), all_tokens, jnp.int32).at[expert_of, place].set(token_of)
    rounded = lax.optimization_barrier(route_weights.astype(jnp.bfloat16)).astype(jnp.float32).reshape(-1)
    weight_table = jnp.zeros((experts, slot_count), jnp.float32).at[expert_of, place].set(rounded)
    padded_rows = jnp.concatenate([tokens, jnp.zeros((1, D), jnp.bfloat16)], 0)
    padded_back = jnp.concatenate([cotangent, jnp.zeros((1, D), jnp.bfloat16)], 0)
    hidden_block = F // N_TP

    def one_expert(args):
        index, weight, wgate, wup, wdown = args
        rows = padded_rows[index]
        back = padded_back[index]
        weight = weight[:, None]
        pre_gate = jnp.dot(rows, wgate, preferred_element_type=jnp.float32)
        pre_up = jnp.dot(rows, wup, preferred_element_type=jnp.float32)
        along = jnp.dot(back, wdown.T, preferred_element_type=jnp.float32)
        gate_sig = jax.nn.sigmoid(pre_gate)
        gate_act = pre_gate * gate_sig
        hidden = gate_act * pre_up
        hidden_grad = weight * along
        gate_grad = (hidden_grad * pre_up * gate_sig * (1.0 + pre_gate * (1.0 - gate_sig))).astype(jnp.bfloat16)
        up_grad = (hidden_grad * gate_act).astype(jnp.bfloat16)
        scaled = (weight * hidden).astype(jnp.bfloat16)
        grad_gate = jnp.dot(rows.T, gate_grad, preferred_element_type=jnp.float32).astype(jnp.bfloat16)
        grad_up = jnp.dot(rows.T, up_grad, preferred_element_type=jnp.float32).astype(jnp.bfloat16)
        grad_down = jnp.dot(scaled.T, back, preferred_element_type=jnp.float32).astype(jnp.bfloat16)
        slot_total = index.shape[0]
        gate_blocks = gate_grad.astype(jnp.float32).reshape(slot_total, N_TP, hidden_block)
        up_blocks = up_grad.astype(jnp.float32).reshape(slot_total, N_TP, hidden_block)
        wgate_blocks = wgate.astype(jnp.float32).reshape(D, N_TP, hidden_block)
        wup_blocks = wup.astype(jnp.float32).reshape(D, N_TP, hidden_block)
        row_part = jnp.einsum('rbf,dbf->rbd', gate_blocks, wgate_blocks) + jnp.einsum('rbf,dbf->rbd', up_blocks, wup_blocks)
        row_part = lax.optimization_barrier(row_part.astype(jnp.bfloat16)).astype(jnp.float32)
        slot_rows = jnp.sum(row_part, axis=1).astype(jnp.bfloat16)
        slot_part = jnp.sum((hidden * along).reshape(slot_total, N_TP, hidden_block), axis=2)
        slot_part = lax.optimization_barrier(slot_part.astype(jnp.bfloat16)).astype(jnp.float32)
        slot_grad = jnp.sum(slot_part, axis=1).astype(jnp.bfloat16)
        return slot_rows, slot_grad, grad_gate, grad_up, grad_down

    slot_rows, slot_grad, grad_gate, grad_up, grad_down = lax.map(
        one_expert, (table, weight_table, w_gate, w_up, w_down))
    picked = slot_rows[expert_of, place].astype(jnp.float32).reshape(all_tokens, TOP, D)
    grad_tokens = jnp.sum(picked, axis=1).astype(jnp.bfloat16)
    grad_weights = slot_grad[expert_of, place].reshape(all_tokens, TOP)
    return grad_tokens, grad_weights, grad_gate, grad_up, grad_down
```

```python
import functools
import jax
import jax.numpy as jnp
from jax import lax
from jax.experimental import pallas as pl
from jax.experimental.pallas import tpu as pltpu
from jax.sharding import PartitionSpec as P

MESH = pl.DeviceIdType.MESH
CORES = 2
BF = jnp.bfloat16


def place():
    e, t = lax.axis_index("ep"), lax.axis_index("tp")
    return e, t, t // CORES, lax.rem(t, CORES)


def greet(n_ep, n_y, e, t, y, c):
    barrier = pltpu.get_barrier_semaphore()

    def hello(d, carry):
        pl.semaphore_signal(
            barrier, inc=1, device_id=(lax.rem(e + d, n_ep), t), device_id_type=MESH
        )
        return carry

    lax.fori_loop(1, n_ep, hello, 0)
    for j in range(1, n_y):
        other = lax.rem(y + j, n_y) * CORES + c
        pl.semaphore_signal(barrier, inc=1, device_id=(e, other), device_id_type=MESH)
    pl.semaphore_signal(
        barrier, inc=1, device_id=(e, y * CORES + 1 - c), device_id_type=MESH
    )
    pl.semaphore_wait(barrier, n_ep - 1 + n_y - 1 + 1)


def dispatch_kernel(
    n_ep, n_y, send, out, own_sem, ep_s, ep_r, y_s, y_r, c_s, c_r
):
    e, t, y, c = place()
    capp, quarter = send.shape[2], send.shape[3]
    greet(n_ep, n_y, e, t, y, c)
    sibling = (e, y * CORES + 1 - c)

    def zone(source, q):
        return out.at[
            :,
            pl.ds(pl.multiple_of(source * capp, capp), capp),
            pl.ds(pl.multiple_of(q * quarter, quarter), quarter),
        ]

    def over_ep(d):
        to = lax.rem(e + d, n_ep)
        return pltpu.make_async_remote_copy(
            send.at[to], zone(e, t), ep_s.at[d], ep_r.at[d], (to, t), MESH
        )

    def ep_landed(d):
        source = lax.rem(e - d + n_ep, n_ep)
        pltpu.make_async_copy(zone(source, t), zone(source, t), ep_r.at[d]).wait()

    def over_y(d, j):
        source = lax.rem(e - d + n_ep, n_ep)
        to = lax.rem(y + j, n_y) * CORES + c
        return pltpu.make_async_remote_copy(
            zone(source, t), zone(source, t), y_s.at[j, d], y_r.at[j, d], (e, to), MESH
        )

    def y_landed(d, j):
        source = lax.rem(e - d + n_ep, n_ep)
        q = lax.rem(y - j + n_y, n_y) * CORES + c
        pltpu.make_async_copy(zone(source, q), zone(source, q), y_r.at[j, d]).wait()

    def over_core(d, j):
        source = lax.rem(e - d + n_ep, n_ep)
        q = lax.rem(y - j + n_y, n_y) * CORES + c
        return pltpu.make_async_remote_copy(
            zone(source, q), zone(source, q), c_s.at[j, d], c_r.at[j, d], sibling, MESH
        )

    def core_landed(d, j):
        source = lax.rem(e - d + n_ep, n_ep)
        q = lax.rem(y - j + n_y, n_y) * CORES + 1 - c
        pltpu.make_async_copy(zone(source, q), zone(source, q), c_r.at[j, d]).wait()

    own = pltpu.make_async_copy(send.at[e], zone(e, t), own_sem)
    own.start()

    def start_ep(d, carry):
        over_ep(d).start()
        return carry

    lax.fori_loop(1, n_ep, start_ep, 0)
    own.wait()
    for j in range(1, n_y):
        over_y(0, j).start()
    over_core(0, 0).start()

    def step(d, carry):
        ep_landed(d)
        for j in range(1, n_y):
            over_y(d, j).start()
        over_core(d, 0).start()
        for j in range(1, n_y):
            y_landed(d - 1, j)
            over_core(d - 1, j).start()
        return carry

    lax.fori_loop(1, n_ep, step, 0)
    for j in range(1, n_y):
        y_landed(n_ep - 1, j)
        over_core(n_ep - 1, j).start()

    def finish(d, carry):
        for j in range(n_y):
            core_landed(d, j)
            over_core(d, j).wait_send()
        for j in range(1, n_y):
            over_y(d, j).wait_send()
        return carry

    lax.fori_loop(0, n_ep, finish, 0)

    def finish_ep(d, carry):
        over_ep(d).wait_send()
        return carry

    lax.fori_loop(1, n_ep, finish_ep, 0)


def dispatch(send, n_ep, n_tp):
    n_y = n_tp // CORES
    capp, quarter = send.shape[2], send.shape[3]
    return pl.pallas_call(
        functools.partial(dispatch_kernel, n_ep, n_y),
        out_shape=jax.ShapeDtypeStruct((2, n_ep * capp, quarter * n_tp), BF),
        in_specs=[pl.BlockSpec(memory_space=pltpu.VMEM)],
        out_specs=pl.BlockSpec(memory_space=pltpu.VMEM),
        scratch_shapes=[
            pltpu.SemaphoreType.DMA,
            pltpu.SemaphoreType.DMA((n_ep,)),
            pltpu.SemaphoreType.DMA((n_ep,)),
            pltpu.SemaphoreType.DMA((n_y, n_ep)),
            pltpu.SemaphoreType.DMA((n_y, n_ep)),
            pltpu.SemaphoreType.DMA((n_y, n_ep)),
            pltpu.SemaphoreType.DMA((n_y, n_ep)),
        ],
        compiler_params=pltpu.CompilerParams(collective_id=0, has_side_effects=True),
        name="dispatch",
    )(send)


def combine_kernel(
    n_ep,
    n_y,
    cap,
    part,
    pick,
    tokens_out,
    slots_out,
    from_core,
    pair,
    from_y,
    total,
    home,
    a_s,
    a_r,
    b_s,
    b_r,
    h_s,
    h_r,
    g_s,
    g_r,
    k_s,
    k_r,
):
    e, t, y, c = place()
    capp, quarter = home.shape[1], home.shape[2]
    greet(n_ep, n_y, e, t, y, c)
    sibling = (e, y * CORES + 1 - c)

    def zone(b, q):
        return part.at[
            pl.ds(pl.multiple_of(b * capp, capp), capp),
            pl.ds(pl.multiple_of(q * quarter, quarter), quarter),
        ]

    def block(d):
        return lax.rem(e + d, n_ep)

    def to_core(d, j):
        q = lax.rem(y + j, n_y) * CORES + 1 - c
        return pltpu.make_async_remote_copy(
            zone(block(d), q), from_core.at[j, d], a_s.at[j, d], a_r.at[j, d], sibling, MESH
        )

    def to_y(d, j):
        q = lax.rem(y + j, n_y) * CORES + c
        return pltpu.make_async_remote_copy(
            pair.at[j, d], from_y.at[j, d], b_s.at[j, d], b_r.at[j, d], (e, q), MESH
        )

    def to_home(d):
        return pltpu.make_async_remote_copy(
            total.at[d], home.at[e], h_s.at[d], h_r.at[d], (block(d), t), MESH
        )

    def mine(d, j):
        q = lax.rem(y + j, n_y) * CORES + c
        return zone(block(d), q)[...].astype(jnp.float32) + from_core[j, d].astype(
            jnp.float32
        )

    def first(d, carry):
        for j in range(n_y):
            to_core(d, (j + 1) % n_y).start()
        return carry

    lax.fori_loop(1, n_ep, first, 0)
    first(0, 0)

    def second(d, carry):
        for j in range(1, n_y):
            to_core(d, j).wait()
            pair[j, d] = mine(d, j).astype(BF)
            to_y(d, j).start()
        return carry

    lax.fori_loop(1, n_ep, second, 0)
    second(0, 0)

    def added(d):
        to_core(d, 0).wait()
        value = mine(d, 0)
        for j in range(1, n_y):
            to_y(d, j).wait()
            value = value + from_y[j, d].astype(jnp.float32)
        return value.astype(BF)

    def third(d, carry):
        total[d] = added(d)
        to_home(d).start()
        return carry

    lax.fori_loop(1, n_ep, third, 0)
    home[e] = added(0)

    def landed(d, carry):
        source = lax.rem(e - d + n_ep, n_ep)
        pltpu.make_async_copy(home.at[source], home.at[source], h_r.at[d]).wait()
        return carry

    lax.fori_loop(1, n_ep, landed, 0)

    def columns(q):
        return tokens_out.at[:, pl.ds(pl.multiple_of(q * quarter, quarter), quarter)]

    columns(t)[...] = jnp.dot(
        pick[...],
        home[...].reshape(n_ep * capp, quarter),
        preferred_element_type=jnp.float32,
    ).astype(BF)

    def gather_y(j):
        q = lax.rem(y + j, n_y) * CORES + c
        return pltpu.make_async_remote_copy(
            columns(t), columns(t), g_s.at[j], g_r.at[j], (e, q), MESH
        )

    def gather_core(j):
        q = lax.rem(y - j + n_y, n_y) * CORES + c
        return pltpu.make_async_remote_copy(
            columns(q), columns(q), k_s.at[j], k_r.at[j], sibling, MESH
        )

    for j in range(1, n_y):
        gather_y(j).start()
    gather_core(0).start()
    slots_out[...] = home[:, cap, :]
    for j in range(1, n_y):
        q = lax.rem(y - j + n_y, n_y) * CORES + c
        pltpu.make_async_copy(columns(q), columns(q), g_r.at[j]).wait()
        gather_core(j).start()
    for j in range(n_y):
        q = lax.rem(y - j + n_y, n_y) * CORES + 1 - c
        pltpu.make_async_copy(columns(q), columns(q), k_r.at[j]).wait()
        gather_core(j).wait_send()
    for j in range(1, n_y):
        gather_y(j).wait_send()

    def finish(d, carry):
        to_home(d).wait_send()
        return carry

    lax.fori_loop(1, n_ep, finish, 0)


def combine(part, pick, cap, n_ep, n_tp):
    n_y = n_tp // CORES
    capp = part.shape[0] // n_ep
    width = part.shape[1]
    quarter = width // n_tp
    dma = pltpu.SemaphoreType.DMA
    vmem = pl.BlockSpec(memory_space=pltpu.VMEM)
    return pl.pallas_call(
        functools.partial(combine_kernel, n_ep, n_y, cap),
        out_shape=(
            jax.ShapeDtypeStruct((pick.shape[0], width), BF),
            jax.ShapeDtypeStruct((n_ep, quarter), BF),
        ),
        in_specs=[vmem, vmem],
        out_specs=(vmem, vmem),
        scratch_shapes=[
            pltpu.VMEM((n_y, n_ep, capp, quarter), BF),
            pltpu.VMEM((n_y, n_ep, capp, quarter), BF),
            pltpu.VMEM((n_y, n_ep, capp, quarter), BF),
            pltpu.VMEM((n_ep, capp, quarter), BF),
            pltpu.VMEM((n_ep, capp, quarter), BF),
            dma((n_y, n_ep)),
            dma((n_y, n_ep)),
            dma((n_y, n_ep)),
            dma((n_y, n_ep)),
            dma((n_ep,)),
            dma((n_ep,)),
            dma((n_y,)),
            dma((n_y,)),
            dma((n_y,)),
            dma((n_y,)),
        ],
        compiler_params=pltpu.CompilerParams(collective_id=1, has_side_effects=True),
        name="combine",
    )(part, pick)


def on_device(tokens, cotangent, routing, route_weights, w_gate, w_up, w_down):
    n_ep, n_tp = lax.axis_size("ep"), lax.axis_size("tp")
    t = lax.axis_index("tp")
    local_tokens, top_count = routing.shape
    width = tokens.shape[1]
    quarter = width // n_tp
    cap = max(2, (5 * local_tokens * top_count + 4 * n_ep - 1) // (4 * n_ep))
    capp = (cap + 1 + 15) // 16 * 16
    slots = n_ep * capp
    experts = jnp.arange(n_ep, dtype=jnp.int32)
    named = [routing[:, k, None] == experts[None, :] for k in range(top_count)]
    any_named = functools.reduce(jnp.logical_or, named)
    order = jnp.arange(local_tokens, dtype=jnp.int32)
    earlier = (order[:, None] > order[None, :]).astype(BF)
    before = jnp.dot(earlier, any_named.astype(BF), preferred_element_type=jnp.float32)
    targets = [
        jnp.sum(
            jnp.where(n, before.astype(jnp.int32) + experts[None, :] * capp, 0), axis=1
        )
        for n in named
    ]
    slot_ids = jnp.arange(slots, dtype=jnp.int32)
    chosen = [target[:, None] == slot_ids[None, :] for target in targets]
    pick = functools.reduce(jnp.logical_or, chosen).astype(BF)
    slot_weight = sum(
        jnp.sum(jnp.where(ch, route_weights[:, k, None], 0.0), axis=0)
        for k, ch in enumerate(chosen)
    ).astype(BF)
    spare = (jnp.arange(capp) == cap)[None, :, None]

    mine = jnp.concatenate(
        [
            lax.dynamic_slice_in_dim(tokens, t * quarter, quarter, 1)[None],
            lax.dynamic_slice_in_dim(cotangent, t * quarter, quarter, 1)[None],
        ],
        0,
    )
    sent = jnp.einsum("ts,atd->asd", pick, mine, preferred_element_type=jnp.float32).astype(BF)
    sent = sent.reshape(2, n_ep, capp, quarter)
    weight_row = jnp.pad(slot_weight.reshape(n_ep, 1, capp), ((0, 0), (0, 0), (0, quarter - capp)))
    send = jnp.stack([jnp.where(spare, weight_row, sent[0]), sent[1]], axis=1)

    both = dispatch(send, n_ep, n_tp)
    rows, back = both[0], both[1]
    weight = rows.reshape(n_ep, capp, width)[:, cap, :capp].reshape(slots, 1).astype(jnp.float32)
    wgate, wup, wdown = w_gate[0], w_up[0], w_down[0]
    pre_gate = jnp.dot(rows, wgate, preferred_element_type=jnp.float32)
    pre_up = jnp.dot(rows, wup, preferred_element_type=jnp.float32)
    along = jnp.einsum("rd,fd->rf", back, wdown, preferred_element_type=jnp.float32)
    gate_sig = jax.nn.sigmoid(pre_gate)
    gate_act = pre_gate * gate_sig
    hidden = gate_act * pre_up
    hidden_grad = weight * along
    gate_grad = (hidden_grad * pre_up * gate_sig * (1.0 + pre_gate * (1.0 - gate_sig))).astype(BF)
    up_grad = (hidden_grad * gate_act).astype(BF)
    scaled = (weight * hidden).astype(BF)
    row_part = jnp.einsum(
        "rf,df->rd", gate_grad, wgate, preferred_element_type=jnp.float32
    ) + jnp.einsum("rf,df->rd", up_grad, wup, preferred_element_type=jnp.float32)
    slot_part = jnp.sum(hidden * along, axis=1).astype(BF)
    slot_row = jnp.pad(slot_part.reshape(n_ep, 1, capp), ((0, 0), (0, 0), (0, quarter - capp)))
    part = jnp.where(
        spare, jnp.tile(slot_row, (1, 1, n_tp)), row_part.astype(BF).reshape(n_ep, capp, width)
    ).reshape(slots, width)
    grad_tokens, slot_home = combine(part, pick, cap, n_ep, n_tp)
    slot_grad = slot_home[:, :capp].reshape(1, slots).astype(jnp.float32)
    grad_weights = jnp.stack(
        [jnp.sum(jnp.where(ch, slot_grad, 0.0), axis=1) for ch in chosen], axis=1
    ).astype(BF)
    grad_gate = jnp.einsum("rd,rf->df", rows, gate_grad, preferred_element_type=jnp.float32).astype(BF)
    grad_up = jnp.einsum("rd,rf->df", rows, up_grad, preferred_element_type=jnp.float32).astype(BF)
    grad_down = jnp.einsum("rf,rd->fd", scaled, back, preferred_element_type=jnp.float32).astype(BF)
    return (grad_tokens, grad_weights, grad_gate[None], grad_up[None], grad_down[None])


def solution(mesh):
    return jax.shard_map(
        on_device,
        mesh=mesh,
        in_specs=(
            P("ep", None),
            P("ep", None),
            P("ep", None),
            P("ep", None),
            P("ep", None, "tp"),
            P("ep", None, "tp"),
            P("ep", "tp", None),
        ),
        out_specs=(
            P("ep", None),
            P("ep", None),
            P("ep", None, "tp"),
            P("ep", None, "tp"),
            P("ep", "tp", None),
        ),
        check_vma=False,
    )
```

```python
import functools
import jax
import jax.numpy as jnp
from jax import lax
from jax.experimental import pallas as pl
from jax.experimental.pallas import tpu as pltpu
from jax.sharding import PartitionSpec as P

MESH = pl.DeviceIdType.MESH
CORES = 2
BF = jnp.bfloat16


def place():
    e, t = lax.axis_index("ep"), lax.axis_index("tp")
    return e, t, t // CORES, lax.rem(t, CORES)


def partner(e, d, n_ep, back):
    if n_ep & (n_ep - 1):
        return lax.rem(e + n_ep - d, n_ep) if back else lax.rem(e + d, n_ep)
    found, bit = 0, 1
    while bit < n_ep:
        mine, other = lax.rem(e // bit, 2), lax.rem(d // bit, 2)
        found = found + bit * lax.rem(mine + other, 2)
        bit *= 2
    return found


def greet(n_ep, n_y, e, t, y, c):
    barrier = pltpu.get_barrier_semaphore()

    def hello(d, carry):
        pl.semaphore_signal(
            barrier, inc=1, device_id=(lax.rem(e + d, n_ep), t), device_id_type=MESH
        )
        return carry

    lax.fori_loop(1, n_ep, hello, 0)
    for j in range(1, n_y):
        other = lax.rem(y + j, n_y) * CORES + c
        pl.semaphore_signal(barrier, inc=1, device_id=(e, other), device_id_type=MESH)
    pl.semaphore_signal(
        barrier, inc=1, device_id=(e, y * CORES + 1 - c), device_id_type=MESH
    )
    pl.semaphore_wait(barrier, n_ep - 1 + n_y - 1 + 1)


def dispatch_kernel(
    n_ep, n_y, send, out, own_sem, ep_s, ep_r, y_s, y_r, c_s, c_r
):
    e, t, y, c = place()
    capp, quarter = send.shape[2], send.shape[3]
    greet(n_ep, n_y, e, t, y, c)
    sibling = (e, y * CORES + 1 - c)

    def zone(source, q):
        return out.at[
            :,
            pl.ds(pl.multiple_of(source * capp, capp), capp),
            pl.ds(pl.multiple_of(q * quarter, quarter), quarter),
        ]

    def over_ep(d):
        to = partner(e, d, n_ep, False)
        return pltpu.make_async_remote_copy(
            send.at[to], zone(e, t), ep_s.at[d], ep_r.at[d], (to, t), MESH
        )

    def ep_landed(d):
        source = partner(e, d, n_ep, True)
        pltpu.make_async_copy(zone(source, t), zone(source, t), ep_r.at[d]).wait()

    def over_y(d, j):
        source = partner(e, d, n_ep, True)
        to = lax.rem(y + j, n_y) * CORES + c
        return pltpu.make_async_remote_copy(
            zone(source, t), zone(source, t), y_s.at[j, d], y_r.at[j, d], (e, to), MESH
        )

    def y_landed(d, j):
        source = partner(e, d, n_ep, True)
        q = lax.rem(y - j + n_y, n_y) * CORES + c
        pltpu.make_async_copy(zone(source, q), zone(source, q), y_r.at[j, d]).wait()

    def over_core(d, j):
        source = partner(e, d, n_ep, True)
        q = lax.rem(y - j + n_y, n_y) * CORES + c
        return pltpu.make_async_remote_copy(
            zone(source, q), zone(source, q), c_s.at[j, d], c_r.at[j, d], sibling, MESH
        )

    def core_landed(d, j):
        source = partner(e, d, n_ep, True)
        q = lax.rem(y - j + n_y, n_y) * CORES + 1 - c
        pltpu.make_async_copy(zone(source, q), zone(source, q), c_r.at[j, d]).wait()

    own = pltpu.make_async_copy(send.at[e], zone(e, t), own_sem)
    own.start()

    def start_ep(d, carry):
        over_ep(d).start()
        return carry

    lax.fori_loop(1, n_ep, start_ep, 0)
    own.wait()
    for j in range(1, n_y):
        over_y(0, j).start()
    over_core(0, 0).start()

    def step(d, carry):
        ep_landed(d)
        for j in range(1, n_y):
            over_y(d, j).start()
        over_core(d, 0).start()
        for j in range(1, n_y):
            y_landed(d - 1, j)
            over_core(d - 1, j).start()
        return carry

    lax.fori_loop(1, n_ep, step, 0)
    for j in range(1, n_y):
        y_landed(n_ep - 1, j)
        over_core(n_ep - 1, j).start()

    def finish(d, carry):
        for j in range(n_y):
            core_landed(d, j)
            over_core(d, j).wait_send()
        for j in range(1, n_y):
            over_y(d, j).wait_send()
        return carry

    lax.fori_loop(0, n_ep, finish, 0)

    def finish_ep(d, carry):
        over_ep(d).wait_send()
        return carry

    lax.fori_loop(1, n_ep, finish_ep, 0)


def dispatch(send, n_ep, n_tp):
    n_y = n_tp // CORES
    capp, quarter = send.shape[2], send.shape[3]
    return pl.pallas_call(
        functools.partial(dispatch_kernel, n_ep, n_y),
        out_shape=jax.ShapeDtypeStruct((2, n_ep * capp, quarter * n_tp), BF),
        in_specs=[pl.BlockSpec(memory_space=pltpu.VMEM)],
        out_specs=pl.BlockSpec(memory_space=pltpu.VMEM),
        scratch_shapes=[
            pltpu.SemaphoreType.DMA,
            pltpu.SemaphoreType.DMA((n_ep,)),
            pltpu.SemaphoreType.DMA((n_ep,)),
            pltpu.SemaphoreType.DMA((n_y, n_ep)),
            pltpu.SemaphoreType.DMA((n_y, n_ep)),
            pltpu.SemaphoreType.DMA((n_y, n_ep)),
            pltpu.SemaphoreType.DMA((n_y, n_ep)),
        ],
        compiler_params=pltpu.CompilerParams(collective_id=0, has_side_effects=True),
        name="dispatch",
    )(send)


def combine_kernel(
    n_ep,
    n_y,
    cap,
    gate_grad,
    up_grad,
    w_gate,
    w_up,
    slot_row,
    pick,
    tokens_out,
    slots_out,
    part,
    from_core,
    pair,
    from_y,
    total,
    home,
    a_s,
    a_r,
    b_s,
    b_r,
    h_s,
    h_r,
    g_s,
    g_r,
    k_s,
    k_r,
):
    e, t, y, c = place()
    capp, quarter = home.shape[1], home.shape[2]
    greet(n_ep, n_y, e, t, y, c)
    sibling = (e, y * CORES + 1 - c)

    def zone(b, q):
        return part.at[
            pl.ds(pl.multiple_of(b * capp, capp), capp),
            pl.ds(pl.multiple_of(q * quarter, quarter), quarter),
        ]

    def block(d):
        return partner(e, d, n_ep, False)

    def to_core(d, j):
        q = lax.rem(y + j, n_y) * CORES + 1 - c
        return pltpu.make_async_remote_copy(
            zone(block(d), q), from_core.at[j, d], a_s.at[j, d], a_r.at[j, d], sibling, MESH
        )

    def to_y(d, j):
        q = lax.rem(y + j, n_y) * CORES + c
        return pltpu.make_async_remote_copy(
            pair.at[j, d], from_y.at[j, d], b_s.at[j, d], b_r.at[j, d], (e, q), MESH
        )

    def to_home(d):
        return pltpu.make_async_remote_copy(
            total.at[d], home.at[e], h_s.at[d], h_r.at[d], (block(d), t), MESH
        )

    def mine(d, j):
        q = lax.rem(y + j, n_y) * CORES + c
        return zone(block(d), q)[...].astype(jnp.float32) + from_core[j, d].astype(
            jnp.float32
        )

    def multiply(q):
        held = pl.ds(pl.multiple_of(q * quarter, quarter), quarter)
        across = (((1,), (1,)), ((), ()))
        value = lax.dot_general(
            gate_grad[...], w_gate[held, :], across, preferred_element_type=jnp.float32
        ) + lax.dot_general(
            up_grad[...], w_up[held, :], across, preferred_element_type=jnp.float32
        )
        value = value.reshape(n_ep, capp, quarter)
        spare = lax.broadcasted_iota(jnp.int32, value.shape, 1) == cap
        value = jnp.where(spare, slot_row[...], value)
        part[:, held] = value.reshape(n_ep * capp, quarter).astype(BF)

    for i in range(n_y):
        j = (i + 1) % n_y
        multiply(lax.rem(y + j, n_y) * CORES + 1 - c)

        def first(i, carry):
            to_core(n_ep - 1 - i, j).start()
            return carry

        lax.fori_loop(0, n_ep, first, 0)
    for i in range(n_y - 1):
        multiply(lax.rem(y + i + 1, n_y) * CORES + c)

    def second(i, carry):
        d = n_ep - 1 - i
        for j in range(1, n_y):
            to_core(d, j).wait()
            pair[j, d] = mine(d, j).astype(BF)
            to_y(d, j).start()
        return carry

    lax.fori_loop(0, n_ep, second, 0)
    multiply(y * CORES + c)

    def added(d):
        to_core(d, 0).wait()
        value = mine(d, 0)
        for j in range(1, n_y):
            to_y(d, j).wait()
            value = value + from_y[j, d].astype(jnp.float32)
        return value.astype(BF)

    def third(i, carry):
        d = n_ep - i
        total[d] = added(d)
        to_home(d).start()
        return carry

    lax.fori_loop(1, n_ep, third, 0)
    home[e] = added(0)

    def landed(d, carry):
        source = partner(e, d, n_ep, True)
        pltpu.make_async_copy(home.at[source], home.at[source], h_r.at[d]).wait()
        return carry

    lax.fori_loop(1, n_ep, landed, 0)

    def columns(q):
        return tokens_out.at[:, pl.ds(pl.multiple_of(q * quarter, quarter), quarter)]

    columns(t)[...] = jnp.dot(
        pick[...],
        home[...].reshape(n_ep * capp, quarter),
        preferred_element_type=jnp.float32,
    ).astype(BF)

    def gather_y(j):
        q = lax.rem(y + j, n_y) * CORES + c
        return pltpu.make_async_remote_copy(
            columns(t), columns(t), g_s.at[j], g_r.at[j], (e, q), MESH
        )

    def gather_core(j):
        q = lax.rem(y - j + n_y, n_y) * CORES + c
        return pltpu.make_async_remote_copy(
            columns(q), columns(q), k_s.at[j], k_r.at[j], sibling, MESH
        )

    for j in range(1, n_y):
        gather_y(j).start()
    gather_core(0).start()
    slots_out[...] = home[:, cap, :]
    for j in range(1, n_y):
        q = lax.rem(y - j + n_y, n_y) * CORES + c
        pltpu.make_async_copy(columns(q), columns(q), g_r.at[j]).wait()
        gather_core(j).start()
    for j in range(n_y):
        q = lax.rem(y - j + n_y, n_y) * CORES + 1 - c
        pltpu.make_async_copy(columns(q), columns(q), k_r.at[j]).wait()
        gather_core(j).wait_send()
    for j in range(1, n_y):
        gather_y(j).wait_send()

    def finish(d, carry):
        to_home(d).wait_send()
        return carry

    lax.fori_loop(1, n_ep, finish, 0)


def combine(gate_grad, up_grad, w_gate, w_up, slot_row, pick, cap, n_ep, n_tp):
    n_y = n_tp // CORES
    capp = gate_grad.shape[0] // n_ep
    width = w_gate.shape[0]
    quarter = width // n_tp
    dma = pltpu.SemaphoreType.DMA
    vmem = pl.BlockSpec(memory_space=pltpu.VMEM)
    return pl.pallas_call(
        functools.partial(combine_kernel, n_ep, n_y, cap),
        out_shape=(
            jax.ShapeDtypeStruct((pick.shape[0], width), BF),
            jax.ShapeDtypeStruct((n_ep, quarter), BF),
        ),
        in_specs=[vmem] * 6,
        out_specs=(vmem, vmem),
        scratch_shapes=[
            pltpu.VMEM((n_ep * capp, width), BF),
            pltpu.VMEM((n_y, n_ep, capp, quarter), BF),
            pltpu.VMEM((n_y, n_ep, capp, quarter), BF),
            pltpu.VMEM((n_y, n_ep, capp, quarter), BF),
            pltpu.VMEM((n_ep, capp, quarter), BF),
            pltpu.VMEM((n_ep, capp, quarter), BF),
            dma((n_y, n_ep)),
            dma((n_y, n_ep)),
            dma((n_y, n_ep)),
            dma((n_y, n_ep)),
            dma((n_ep,)),
            dma((n_ep,)),
            dma((n_y,)),
            dma((n_y,)),
            dma((n_y,)),
            dma((n_y,)),
        ],
        compiler_params=pltpu.CompilerParams(collective_id=1, has_side_effects=True),
        name="combine",
    )(gate_grad, up_grad, w_gate, w_up, slot_row, pick)


def on_device(tokens, cotangent, routing, route_weights, w_gate, w_up, w_down):
    n_ep, n_tp = lax.axis_size("ep"), lax.axis_size("tp")
    t = lax.axis_index("tp")
    local_tokens, top_count = routing.shape
    width = tokens.shape[1]
    quarter = width // n_tp
    cap = max(2, (5 * local_tokens * top_count + 4 * n_ep - 1) // (4 * n_ep))
    capp = (cap + 1 + 15) // 16 * 16
    slots = n_ep * capp
    experts = jnp.arange(n_ep, dtype=jnp.int32)
    named = [routing[:, k, None] == experts[None, :] for k in range(top_count)]
    any_named = functools.reduce(jnp.logical_or, named)
    order = jnp.arange(local_tokens, dtype=jnp.int32)
    earlier = (order[:, None] > order[None, :]).astype(BF)
    before = jnp.dot(earlier, any_named.astype(BF), preferred_element_type=jnp.float32)
    targets = [
        jnp.sum(
            jnp.where(n, before.astype(jnp.int32) + experts[None, :] * capp, 0), axis=1
        )
        for n in named
    ]
    slot_ids = jnp.arange(slots, dtype=jnp.int32)
    chosen = [target[:, None] == slot_ids[None, :] for target in targets]
    pick = functools.reduce(jnp.logical_or, chosen).astype(BF)
    slot_weight = sum(
        jnp.sum(jnp.where(ch, route_weights[:, k, None], 0.0), axis=0)
        for k, ch in enumerate(chosen)
    ).astype(BF)
    spare = (jnp.arange(capp) == cap)[None, :, None]

    mine = jnp.concatenate(
        [
            lax.dynamic_slice_in_dim(tokens, t * quarter, quarter, 1)[None],
            lax.dynamic_slice_in_dim(cotangent, t * quarter, quarter, 1)[None],
        ],
        0,
    )
    sent = jnp.einsum("ts,atd->asd", pick, mine, preferred_element_type=jnp.float32).astype(BF)
    sent = sent.reshape(2, n_ep, capp, quarter)
    weight_row = jnp.pad(slot_weight.reshape(n_ep, 1, capp), ((0, 0), (0, 0), (0, quarter - capp)))
    send = jnp.stack([jnp.where(spare, weight_row, sent[0]), sent[1]], axis=1)

    both = dispatch(send, n_ep, n_tp)
    rows, back = both[0], both[1]
    weight = rows.reshape(n_ep, capp, width)[:, cap, :capp].reshape(slots, 1).astype(jnp.float32)
    wgate, wup, wdown = w_gate[0], w_up[0], w_down[0]
    pre_gate = jnp.dot(rows, wgate, preferred_element_type=jnp.float32)
    pre_up = jnp.dot(rows, wup, preferred_element_type=jnp.float32)
    along = jnp.einsum("rd,fd->rf", back, wdown, preferred_element_type=jnp.float32)
    gate_sig = jax.nn.sigmoid(pre_gate)
    gate_act = pre_gate * gate_sig
    hidden = gate_act * pre_up
    hidden_grad = weight * along
    gate_grad = (hidden_grad * pre_up * gate_sig * (1.0 + pre_gate * (1.0 - gate_sig))).astype(BF)
    up_grad = (hidden_grad * gate_act).astype(BF)
    scaled = (weight * hidden).astype(BF)
    slot_part = jnp.sum(hidden * along, axis=1)
    slot_row = jnp.pad(slot_part.reshape(n_ep, 1, capp), ((0, 0), (0, 0), (0, quarter - capp)))
    grad_tokens, slot_home = combine(
        gate_grad, up_grad, wgate, wup, slot_row, pick, cap, n_ep, n_tp
    )
    slot_grad = slot_home[:, :capp].reshape(1, slots).astype(jnp.float32)
    grad_weights = jnp.stack(
        [jnp.sum(jnp.where(ch, slot_grad, 0.0), axis=1) for ch in chosen], axis=1
    ).astype(BF)
    grad_gate = jnp.einsum("rd,rf->df", rows, gate_grad, preferred_element_type=jnp.float32).astype(BF)
    grad_up = jnp.einsum("rd,rf->df", rows, up_grad, preferred_element_type=jnp.float32).astype(BF)
    grad_down = jnp.einsum("rf,rd->fd", scaled, back, preferred_element_type=jnp.float32).astype(BF)
    return (grad_tokens, grad_weights, grad_gate[None], grad_up[None], grad_down[None])


def solution(mesh):
    return jax.shard_map(
        on_device,
        mesh=mesh,
        in_specs=(
            P("ep", None),
            P("ep", None),
            P("ep", None),
            P("ep", None),
            P("ep", None, "tp"),
            P("ep", None, "tp"),
            P("ep", "tp", None),
        ),
        out_specs=(
            P("ep", None),
            P("ep", None),
            P("ep", None, "tp"),
            P("ep", None, "tp"),
            P("ep", "tp", None),
        ),
        check_vma=False,
    )
```

```python
import functools
import jax
import jax.numpy as jnp
from jax import lax
from jax.experimental import pallas as pl
from jax.experimental.pallas import tpu as pltpu
from jax.sharding import PartitionSpec as P

MESH = pl.DeviceIdType.MESH
CORES = 2
BF = jnp.bfloat16


def place():
    e, t = lax.axis_index("ep"), lax.axis_index("tp")
    return e, t, t // CORES, lax.rem(t, CORES)


def partner(e, d, n_ep, back):
    if n_ep & (n_ep - 1):
        return lax.rem(e + n_ep - d, n_ep) if back else lax.rem(e + d, n_ep)
    found, bit = 0, 1
    while bit < n_ep:
        mine, other = lax.rem(e // bit, 2), lax.rem(d // bit, 2)
        found = found + bit * lax.rem(mine + other, 2)
        bit *= 2
    return found


def greet(n_ep, n_y, e, t, y, c):
    barrier = pltpu.get_barrier_semaphore()

    def hello(d, carry):
        pl.semaphore_signal(
            barrier, inc=1, device_id=(lax.rem(e + d, n_ep), t), device_id_type=MESH
        )
        return carry

    lax.fori_loop(1, n_ep, hello, 0)
    for j in range(1, n_y):
        other = lax.rem(y + j, n_y) * CORES + c
        pl.semaphore_signal(barrier, inc=1, device_id=(e, other), device_id_type=MESH)
    pl.semaphore_signal(
        barrier, inc=1, device_id=(e, y * CORES + 1 - c), device_id_type=MESH
    )
    pl.semaphore_wait(barrier, n_ep - 1 + n_y - 1 + 1)


def dispatch_kernel(
    n_ep, n_y, send, out, own_sem, ep_s, ep_r, y_s, y_r, c_s, c_r
):
    e, t, y, c = place()
    capp, quarter = send.shape[2], send.shape[3]
    greet(n_ep, n_y, e, t, y, c)
    sibling = (e, y * CORES + 1 - c)

    def zone(source, q):
        return out.at[
            :,
            pl.ds(pl.multiple_of(source * capp, capp), capp),
            pl.ds(pl.multiple_of(q * quarter, quarter), quarter),
        ]

    def over_ep(d):
        to = partner(e, d, n_ep, False)
        return pltpu.make_async_remote_copy(
            send.at[to], zone(e, t), ep_s.at[d], ep_r.at[d], (to, t), MESH
        )

    def ep_landed(d):
        source = partner(e, d, n_ep, True)
        pltpu.make_async_copy(zone(source, t), zone(source, t), ep_r.at[d]).wait()

    def over_y(d, j):
        source = partner(e, d, n_ep, True)
        to = lax.rem(y + j, n_y) * CORES + c
        return pltpu.make_async_remote_copy(
            zone(source, t), zone(source, t), y_s.at[j, d], y_r.at[j, d], (e, to), MESH
        )

    def y_landed(d, j):
        source = partner(e, d, n_ep, True)
        q = lax.rem(y - j + n_y, n_y) * CORES + c
        pltpu.make_async_copy(zone(source, q), zone(source, q), y_r.at[j, d]).wait()

    def over_core(d, j):
        source = partner(e, d, n_ep, True)
        q = lax.rem(y - j + n_y, n_y) * CORES + c
        return pltpu.make_async_remote_copy(
            zone(source, q), zone(source, q), c_s.at[j, d], c_r.at[j, d], sibling, MESH
        )

    def core_landed(d, j):
        source = partner(e, d, n_ep, True)
        q = lax.rem(y - j + n_y, n_y) * CORES + 1 - c
        pltpu.make_async_copy(zone(source, q), zone(source, q), c_r.at[j, d]).wait()

    own = pltpu.make_async_copy(send.at[e], zone(e, t), own_sem)
    own.start()

    def start_ep(d, carry):
        over_ep(d).start()
        return carry

    lax.fori_loop(1, n_ep, start_ep, 0)
    own.wait()
    for j in range(1, n_y):
        over_y(0, j).start()
    over_core(0, 0).start()

    def step(d, carry):
        ep_landed(d)
        for j in range(1, n_y):
            over_y(d, j).start()
        over_core(d, 0).start()
        for j in range(1, n_y):
            y_landed(d - 1, j)
            over_core(d - 1, j).start()
        return carry

    lax.fori_loop(1, n_ep, step, 0)
    for j in range(1, n_y):
        y_landed(n_ep - 1, j)
        over_core(n_ep - 1, j).start()

    def finish(d, carry):
        for j in range(n_y):
            core_landed(d, j)
            over_core(d, j).wait_send()
        for j in range(1, n_y):
            over_y(d, j).wait_send()
        return carry

    lax.fori_loop(0, n_ep, finish, 0)

    def finish_ep(d, carry):
        over_ep(d).wait_send()
        return carry

    lax.fori_loop(1, n_ep, finish_ep, 0)


def dispatch(send, n_ep, n_tp):
    n_y = n_tp // CORES
    capp, quarter = send.shape[2], send.shape[3]
    return pl.pallas_call(
        functools.partial(dispatch_kernel, n_ep, n_y),
        out_shape=jax.ShapeDtypeStruct((2, n_ep * capp, quarter * n_tp), BF),
        in_specs=[pl.BlockSpec(memory_space=pltpu.VMEM)],
        out_specs=pl.BlockSpec(memory_space=pl.ANY),
        scratch_shapes=[
            pltpu.SemaphoreType.DMA,
            pltpu.SemaphoreType.DMA((n_ep,)),
            pltpu.SemaphoreType.DMA((n_ep,)),
            pltpu.SemaphoreType.DMA((n_y, n_ep)),
            pltpu.SemaphoreType.DMA((n_y, n_ep)),
            pltpu.SemaphoreType.DMA((n_y, n_ep)),
            pltpu.SemaphoreType.DMA((n_y, n_ep)),
        ],
        compiler_params=pltpu.CompilerParams(
            collective_id=0, has_side_effects=True, vmem_limit_bytes=8 << 20
        ),
        name="dispatch",
    )(send)


def combine_kernel(
    n_ep,
    n_y,
    cap,
    gate_grad,
    up_grad,
    w_gate,
    w_up,
    slot_row,
    pick,
    tokens_out,
    slots_out,
    part,
    from_core,
    pair,
    from_y,
    total,
    home,
    a_s,
    a_r,
    b_s,
    b_r,
    h_s,
    h_r,
    g_s,
    g_r,
    k_s,
    k_r,
):
    e, t, y, c = place()
    capp, quarter = home.shape[1], home.shape[2]
    greet(n_ep, n_y, e, t, y, c)
    sibling = (e, y * CORES + 1 - c)

    def zone(b, q):
        return part.at[
            pl.ds(pl.multiple_of(b * capp, capp), capp),
            pl.ds(pl.multiple_of(q * quarter, quarter), quarter),
        ]

    def block(d):
        return partner(e, d, n_ep, False)

    def to_core(d, j):
        q = lax.rem(y + j, n_y) * CORES + 1 - c
        return pltpu.make_async_remote_copy(
            zone(block(d), q), from_core.at[j, d], a_s.at[j, d], a_r.at[j, d], sibling, MESH
        )

    def to_y(d, j):
        q = lax.rem(y + j, n_y) * CORES + c
        return pltpu.make_async_remote_copy(
            pair.at[j, d], from_y.at[j, d], b_s.at[j, d], b_r.at[j, d], (e, q), MESH
        )

    def to_home(d):
        return pltpu.make_async_remote_copy(
            total.at[d], home.at[e], h_s.at[d], h_r.at[d], (block(d), t), MESH
        )

    def mine(d, j):
        q = lax.rem(y + j, n_y) * CORES + c
        return zone(block(d), q)[...].astype(jnp.float32) + from_core[j, d].astype(
            jnp.float32
        )

    def multiply(q):
        held = pl.ds(pl.multiple_of(q * quarter, quarter), quarter)
        across = (((1,), (1,)), ((), ()))
        value = lax.dot_general(
            gate_grad[...], w_gate[held, :], across, preferred_element_type=jnp.float32
        ) + lax.dot_general(
            up_grad[...], w_up[held, :], across, preferred_element_type=jnp.float32
        )
        value = value.reshape(n_ep, capp, quarter)
        spare = lax.broadcasted_iota(jnp.int32, value.shape, 1) == cap
        value = jnp.where(spare, slot_row[...], value)
        part[:, held] = value.reshape(n_ep * capp, quarter).astype(BF)

    for i in range(n_y):
        j = (i + 1) % n_y
        multiply(lax.rem(y + j, n_y) * CORES + 1 - c)

        def first(i, carry):
            to_core(n_ep - 1 - i, j).start()
            return carry

        lax.fori_loop(0, n_ep, first, 0)
    for i in range(n_y - 1):
        multiply(lax.rem(y + i + 1, n_y) * CORES + c)

    def second(i, carry):
        d = n_ep - 1 - i
        for j in range(1, n_y):
            to_core(d, j).wait()
            pair[j, d] = mine(d, j).astype(BF)
            to_y(d, j).start()
        return carry

    lax.fori_loop(0, n_ep, second, 0)
    multiply(y * CORES + c)

    def added(d):
        to_core(d, 0).wait()
        value = mine(d, 0)
        for j in range(1, n_y):
            to_y(d, j).wait()
            value = value + from_y[j, d].astype(jnp.float32)
        return value.astype(BF)

    def third(i, carry):
        d = n_ep - i
        total[d] = added(d)
        to_home(d).start()
        return carry

    lax.fori_loop(1, n_ep, third, 0)
    home[e] = added(0)

    def landed(d, carry):
        source = partner(e, d, n_ep, True)
        pltpu.make_async_copy(home.at[source], home.at[source], h_r.at[d]).wait()
        return carry

    lax.fori_loop(1, n_ep, landed, 0)

    def columns(q):
        return tokens_out.at[:, pl.ds(pl.multiple_of(q * quarter, quarter), quarter)]

    columns(t)[...] = jnp.dot(
        pick[...],
        home[...].reshape(n_ep * capp, quarter),
        preferred_element_type=jnp.float32,
    ).astype(BF)

    def gather_y(j):
        q = lax.rem(y + j, n_y) * CORES + c
        return pltpu.make_async_remote_copy(
            columns(t), columns(t), g_s.at[j], g_r.at[j], (e, q), MESH
        )

    def gather_core(j):
        q = lax.rem(y - j + n_y, n_y) * CORES + c
        return pltpu.make_async_remote_copy(
            columns(q), columns(q), k_s.at[j], k_r.at[j], sibling, MESH
        )

    for j in range(1, n_y):
        gather_y(j).start()
    gather_core(0).start()
    slots_out[...] = home[:, cap, :]
    for j in range(1, n_y):
        q = lax.rem(y - j + n_y, n_y) * CORES + c
        pltpu.make_async_copy(columns(q), columns(q), g_r.at[j]).wait()
        gather_core(j).start()
    for j in range(n_y):
        q = lax.rem(y - j + n_y, n_y) * CORES + 1 - c
        pltpu.make_async_copy(columns(q), columns(q), k_r.at[j]).wait()
        gather_core(j).wait_send()
    for j in range(1, n_y):
        gather_y(j).wait_send()

    def finish(d, carry):
        to_home(d).wait_send()
        return carry

    lax.fori_loop(1, n_ep, finish, 0)


def combine(gate_grad, up_grad, w_gate, w_up, slot_row, pick, cap, n_ep, n_tp):
    n_y = n_tp // CORES
    capp = gate_grad.shape[0] // n_ep
    width = w_gate.shape[0]
    quarter = width // n_tp
    dma = pltpu.SemaphoreType.DMA
    vmem = pl.BlockSpec(memory_space=pltpu.VMEM)
    return pl.pallas_call(
        functools.partial(combine_kernel, n_ep, n_y, cap),
        out_shape=(
            jax.ShapeDtypeStruct((pick.shape[0], width), BF),
            jax.ShapeDtypeStruct((n_ep, quarter), BF),
        ),
        in_specs=[vmem] * 6,
        out_specs=(vmem, vmem),
        scratch_shapes=[
            pltpu.VMEM((n_ep * capp, width), BF),
            pltpu.VMEM((n_y, n_ep, capp, quarter), BF),
            pltpu.VMEM((n_y, n_ep, capp, quarter), BF),
            pltpu.VMEM((n_y, n_ep, capp, quarter), BF),
            pltpu.VMEM((n_ep, capp, quarter), BF),
            pltpu.VMEM((n_ep, capp, quarter), BF),
            dma((n_y, n_ep)),
            dma((n_y, n_ep)),
            dma((n_y, n_ep)),
            dma((n_y, n_ep)),
            dma((n_ep,)),
            dma((n_ep,)),
            dma((n_y,)),
            dma((n_y,)),
            dma((n_y,)),
            dma((n_y,)),
        ],
        compiler_params=pltpu.CompilerParams(collective_id=1, has_side_effects=True),
        name="combine",
    )(gate_grad, up_grad, w_gate, w_up, slot_row, pick)


def on_device(tokens, cotangent, routing, route_weights, w_gate, w_up, w_down):
    n_ep, n_tp = lax.axis_size("ep"), lax.axis_size("tp")
    t = lax.axis_index("tp")
    local_tokens, top_count = routing.shape
    width = tokens.shape[1]
    quarter = width // n_tp
    cap = max(2, (5 * local_tokens * top_count + 4 * n_ep - 1) // (4 * n_ep))
    capp = (cap + 1 + 15) // 16 * 16
    slots = n_ep * capp
    experts = jnp.arange(n_ep, dtype=jnp.int32)
    named = [routing[:, k, None] == experts[None, :] for k in range(top_count)]
    any_named = functools.reduce(jnp.logical_or, named)
    order = jnp.arange(local_tokens, dtype=jnp.int32)
    earlier = (order[:, None] > order[None, :]).astype(BF)
    before = jnp.dot(earlier, any_named.astype(BF), preferred_element_type=jnp.float32)
    targets = [
        jnp.sum(
            jnp.where(n, before.astype(jnp.int32) + experts[None, :] * capp, 0), axis=1
        )
        for n in named
    ]
    slot_ids = jnp.arange(slots, dtype=jnp.int32)
    chosen = [target[:, None] == slot_ids[None, :] for target in targets]
    pick = functools.reduce(jnp.logical_or, chosen).astype(BF)
    slot_weight = sum(
        jnp.sum(jnp.where(ch, route_weights[:, k, None], 0.0), axis=0)
        for k, ch in enumerate(chosen)
    ).astype(BF)
    spare = (jnp.arange(capp) == cap)[None, :, None]

    mine = jnp.concatenate(
        [
            lax.dynamic_slice_in_dim(tokens, t * quarter, quarter, 1)[None],
            lax.dynamic_slice_in_dim(cotangent, t * quarter, quarter, 1)[None],
        ],
        0,
    )
    sent = jnp.einsum("ts,atd->asd", pick, mine, preferred_element_type=jnp.float32).astype(BF)
    sent = sent.reshape(2, n_ep, capp, quarter)
    weight_row = jnp.pad(slot_weight.reshape(n_ep, 1, capp), ((0, 0), (0, 0), (0, quarter - capp)))
    send = jnp.stack([jnp.where(spare, weight_row, sent[0]), sent[1]], axis=1)

    both = dispatch(send, n_ep, n_tp)
    rows, back = both[0], both[1]
    weight = rows.reshape(n_ep, capp, width)[:, cap, :capp].reshape(slots, 1).astype(jnp.float32)
    wgate, wup, wdown = w_gate[0], w_up[0], w_down[0]
    pre_gate = jnp.dot(rows, wgate, preferred_element_type=jnp.float32)
    pre_up = jnp.dot(rows, wup, preferred_element_type=jnp.float32)
    along = jnp.einsum("rd,fd->rf", back, wdown, preferred_element_type=jnp.float32)
    gate_sig = jax.nn.sigmoid(pre_gate)
    gate_act = pre_gate * gate_sig
    hidden = gate_act * pre_up
    hidden_grad = weight * along
    gate_grad = (hidden_grad * pre_up * gate_sig * (1.0 + pre_gate * (1.0 - gate_sig))).astype(BF)
    up_grad = (hidden_grad * gate_act).astype(BF)
    scaled = (weight * hidden).astype(BF)
    slot_part = jnp.sum(hidden * along, axis=1)
    slot_row = jnp.pad(slot_part.reshape(n_ep, 1, capp), ((0, 0), (0, 0), (0, quarter - capp)))
    grad_tokens, slot_home = combine(
        gate_grad, up_grad, wgate, wup, slot_row, pick, cap, n_ep, n_tp
    )
    slot_grad = slot_home[:, :capp].reshape(1, slots).astype(jnp.float32)
    grad_weights = jnp.stack(
        [jnp.sum(jnp.where(ch, slot_grad, 0.0), axis=1) for ch in chosen], axis=1
    ).astype(BF)
    grad_gate = jnp.einsum("rd,rf->df", rows, gate_grad, preferred_element_type=jnp.float32).astype(BF)
    grad_up = jnp.einsum("rd,rf->df", rows, up_grad, preferred_element_type=jnp.float32).astype(BF)
    grad_down = jnp.einsum("rf,rd->fd", scaled, back, preferred_element_type=jnp.float32).astype(BF)
    return (grad_tokens, grad_weights, grad_gate[None], grad_up[None], grad_down[None])


def solution(mesh):
    return jax.shard_map(
        on_device,
        mesh=mesh,
        in_specs=(
            P("ep", None),
            P("ep", None),
            P("ep", None),
            P("ep", None),
            P("ep", None, "tp"),
            P("ep", None, "tp"),
            P("ep", "tp", None),
        ),
        out_specs=(
            P("ep", None),
            P("ep", None),
            P("ep", None, "tp"),
            P("ep", None, "tp"),
            P("ep", "tp", None),
        ),
        check_vma=False,
    )
```
